32 devices in a mesh: ep: 8 (over z, x), tp: 4 (over y, core).
Axes of the slice: x: 2, y: 2, z: 4, core: 2. Of those that a mesh axis runs over, the one named last changes fastest.
Arguments:
- tokens: bfloat16 [1024, 2048], P('ep'), may hold values from -6 to 6
- chosen: int32 [8, 8, 7], P('ep'), may hold values from -1 to 127, as said below
- pick_weight: float32 [8, 8, 7], P('ep'), may hold values from 0.2 to 1
- gate_weight: bfloat16 [8, 2048, 4096], P('ep', None, 'tp'), may hold values from -0.125 to 0.125
- up_weight: bfloat16 [8, 2048, 4096], P('ep', None, 'tp'), may hold values from -0.125 to 0.125
- down_weight: bfloat16 [8, 4096, 2048], P('ep', 'tp'), may hold values from -0.09375 to 0.09375
Outputs:
- combined: bfloat16 [1024, 2048], P('ep', 'tp')
The draws below stay inside these ranges and needn't reach their ends.
Inputs may be any that keep to these rules, and one draw needn't show every extreme that they name: `chosen`: within one group and one expert the named positions are distinct, and the filled slots come first. From each group every expert takes at least 3 tokens and at most 7; every expert takes exactly 7 tokens from some group, and exactly 40 tokens in all.
All inputs are finite; a program needn't handle non-finite values.
Results may differ from the reference program's by a relative error of at most 0.019.
Values may be sent and summed in bfloat16 or wider, within the bound.
No kernel may reach another device: no remote copies, remote signals or barrier semaphores. Data moves between devices by JAX's collectives and lax.ppermute only.
A program may use at most 64 MiB of HBM per device.

```python
import math
import jax
import jax.numpy as jnp
from jax import lax

D = 2048
FF = 4096
TOK_DEV = 128
SLOTS = 7
PICK_DEV = 5
EXPERTS = 8
SOURCES = 8
TOKENS = 1024
N_TP = 4


def draw_chosen(key, part):
    key_count, key_order, key_tokens = jax.random.split(key, 3)
    half_count = SOURCES // 2
    spread = SLOTS - PICK_DEV
    excess = jax.random.randint(key_count, (EXPERTS, half_count), 0, spread + 1)
    excess = excess.at[:, 0].set(spread)
    signed = jnp.concatenate([excess, -excess], axis=1)
    shuffle = jax.vmap(lambda subkey: jax.random.permutation(subkey, SOURCES))(jax.random.split(key_order, EXPERTS))
    counts = PICK_DEV + jnp.take_along_axis(signed, shuffle, axis=1)
    counts = jnp.transpose(counts, (1, 0))
    token_keys = jax.random.split(key_tokens, SOURCES * EXPERTS)
    token_perm = jax.vmap(lambda subkey: jax.random.permutation(subkey, TOK_DEV)[:SLOTS])(token_keys)
    token_perm = token_perm.reshape(SOURCES, EXPERTS, SLOTS)
    slot_index = jnp.arange(SLOTS, dtype=jnp.int32)
    return jnp.where(slot_index[None, None, :] < counts[:, :, None], token_perm, -1).astype(jnp.int32)


def steps_of(rng, dims, pieces, least, top_value):
    def one(position, parts):
        draws = jax.random.uniform(jax.random.fold_in(jax.random.fold_in(rng, 6), position), (parts,), jnp.float32, least / len(pieces), top_value / len(pieces))
        return jnp.repeat(jnp.exp(draws), dims[position] // parts).reshape((-1,) + (1,) * (len(dims) - position - 1))

    loudness = one(*pieces[0])
    for cut in pieces[1:]:
        loudness = loudness * one(*cut)
    return loudness


def gaussian(stream_key, extent, scale, reach, shards=(), held_as=jnp.bfloat16):
    entries = jax.random.normal(stream_key, extent, jnp.float32) * scale
    if len(shards) > 0:
        entries = steps_of(stream_key, extent, shards, -0.22, 0.18) * entries
    return jnp.clip(entries, min=-reach, max=reach).astype(held_as)


def setup_inputs(seed: int = 0) -> dict:
    splits = jax.random.split(jax.random.key(seed), 7)
    tokens = gaussian(splits[0], (TOKENS, D), 1.0, 6.0, ((0, 8),))
    chosen = draw_chosen(jax.random.fold_in(splits[6], 71), 0)
    pick_weight = jnp.clip(jnp.exp(math.log(1.0) - 1.609438 * jax.random.uniform(splits[2], (SOURCES, EXPERTS, SLOTS), jnp.float32) ** steps_of(splits[2], (SOURCES, EXPERTS, SLOTS), ((0, 8),), -0.2, 0.2)), 0.2, 1.0)
    gate_weight = gaussian(splits[3], (EXPERTS, D, FF), D ** -0.5, 0.125, ((0, 8), (2, 4)))
    up_weight = gaussian(splits[4], (EXPERTS, D, FF), D ** -0.5, 0.125, ((0, 8), (2, 4)))
    down_weight = gaussian(splits[5], (EXPERTS, FF, D), FF ** -0.5, 0.09375, ((0, 8), (1, 4)))
    return {"tokens": tokens, "chosen": chosen, "pick_weight": pick_weight, "gate_weight": gate_weight, "up_weight": up_weight, "down_weight": down_weight}


def reference(tokens, chosen, pick_weight, gate_weight, up_weight, down_weight):
    filled = chosen >= 0
    offset = (jnp.arange(SOURCES, dtype=jnp.int32) * TOK_DEV)[:, None, None]
    row_ids = (jnp.where(filled, chosen, 0) + offset).astype(jnp.int32)
    row_ids = jnp.transpose(row_ids, (1, 0, 2)).reshape(EXPERTS, SOURCES * SLOTS)
    filled_flat = jnp.transpose(filled, (1, 0, 2)).reshape(EXPERTS, SOURCES * SLOTS)
    block_len = FF // N_TP

    def expert_step(inputs):
        expert_ids, keep_flags, w_gate, w_up, w_down = inputs
        routed = jnp.where(keep_flags[:, None], tokens[expert_ids], jnp.zeros((), tokens.dtype))
        gate_pre = jnp.dot(routed, w_gate, preferred_element_type=jnp.float32)
        up_pre = jnp.dot(routed, w_up, preferred_element_type=jnp.float32)
        hidden = (jax.nn.silu(gate_pre) * up_pre).astype(jnp.bfloat16)
        hidden = lax.optimization_barrier(hidden)
        hidden_wide = hidden.astype(jnp.float32).reshape(-1, N_TP, block_len)
        down_wide = w_down.astype(jnp.float32).reshape(N_TP, block_len, D)
        partial_value = jnp.einsum('rnf,nfd->nrd', hidden_wide, down_wide).astype(jnp.bfloat16)
        partial_value = lax.optimization_barrier(partial_value)
        return jnp.sum(partial_value.astype(jnp.float32), axis=0).astype(jnp.bfloat16)

    results = lax.map(expert_step, (row_ids, filled_flat, gate_weight, up_weight, down_weight))
    weights = jnp.where(filled_flat, jnp.transpose(pick_weight, (1, 0, 2)).reshape(EXPERTS, SOURCES * SLOTS), jnp.zeros((), jnp.float32))
    terms = weights.reshape(-1)[:, None] * results.reshape(-1, D).astype(jnp.float32)
    combined = jnp.zeros((TOKENS, D), jnp.float32).at[row_ids.reshape(-1)].add(terms)
    return combined.astype(jnp.bfloat16)
```

```python
import jax
import jax.numpy as jnp
from jax import lax
from jax.sharding import PartitionSpec as P
PAD = 8
def first(tokens, chosen, n_tp):
    E = chosen.shape[1]; T = tokens.shape[0]
    ids = jnp.pad(chosen[0], ((0, 0), (0, PAD - chosen.shape[2])), constant_values=-1)
    oh = (ids.reshape(-1)[:, None] == lax.iota(jnp.int32, T)[None, :]).astype(jnp.bfloat16)
    picked = jnp.dot(oh, tokens, preferred_element_type=jnp.float32).astype(jnp.bfloat16)
    return ids, picked.reshape(E, PAD, -1)
def ffn(rows, gw, uw, dw):
    g = jnp.dot(rows, gw[0], preferred_element_type=jnp.float32)
    u = jnp.dot(rows, uw[0], preferred_element_type=jnp.float32)
    h = (jax.nn.silu(g) * u).astype(jnp.bfloat16)
    return jnp.dot(h, dw[0], preferred_element_type=jnp.float32).astype(jnp.bfloat16)
def weights(ids, pw, T):
    w = jnp.pad(pw[0], ((0, 0), (0, PAD - pw.shape[2])))
    return jnp.where(lax.iota(jnp.int32, T)[:, None, None] == ids[None], w[None], 0.0)
def perm_a2a(x, axis):
    n = lax.axis_size(axis)
    i = lax.axis_index(axis)
    parts = [None] * n
    outs = [lax.dynamic_index_in_dim(x, i, 0, keepdims=False)]
    for d in range(1, n):
        send = lax.dynamic_index_in_dim(x, (i + d) % n, 0, keepdims=False)
        outs.append(lax.ppermute(send, axis, [(s, (s + d) % n) for s in range(n)]))
    src = (i - jnp.arange(n)) % n
    return outs, src
def on_device(tokens, chosen, pw, gw, uw, dw):
    n_tp = lax.axis_size("tp")
    E = chosen.shape[1]; T = tokens.shape[0]; D = tokens.shape[1]
    F = D // n_tp
    ids, picked = first(tokens, chosen, n_tp)
    received = lax.all_to_all(picked, "ep", split_axis=0, concat_axis=0, tiled=True)
    rows = received.reshape(-1, D)
    part = ffn(rows, gw, uw, dw)
    p4 = part.reshape(E, PAD, n_tp, F).transpose(0, 2, 1, 3).reshape(E * n_tp, PAD, F)
    got = lax.all_to_all(p4, ("ep", "tp"), split_axis=0, concat_axis=0, tiled=True)
    w = weights(ids, pw, T)
    w = jnp.broadcast_to(w[:, :, None, :], (T, E, n_tp, PAD)).reshape(T, -1)
    return jnp.dot(w, got.reshape(-1, F).astype(jnp.float32), precision=lax.Precision.HIGHEST, preferred_element_type=jnp.float32).astype(jnp.bfloat16)
def solution(mesh):
    return jax.shard_map(on_device, mesh=mesh,
        in_specs=(P("ep", None), P("ep", None, None), P("ep", None, None), P("ep", None, "tp"), P("ep", None, "tp"), P("ep", "tp", None)),
        out_specs=P("ep", "tp"), check_vma=False)
```

```python
import jax
import jax.numpy as jnp
from jax import lax
from jax.experimental import pallas as pl
from jax.experimental.pallas import tpu as pltpu
from jax.sharding import PartitionSpec as P

SUB = 8
CHUNK = 512


def start_all(copies):
    for c in copies:
        c.start()


def half_copies(start, half, width, gate, up, gate_v, up_v, sem):
    n = gate_v.shape[0]
    copies = []
    for c in range(n):
        for k, (src, dst) in enumerate(((gate, gate_v), (up, up_v))):
            where = src.at[0, pl.ds(pl.multiple_of(start, 128), half), pl.ds(c * width, width)]
            copies.append(pltpu.make_async_copy(where, dst.at[c], sem.at[2 * c + k]))
    return copies


def own_body(rows, gate, up, g_out, u_out, gate_v, up_v, sem):
    n, half, width = gate_v.shape
    copies = half_copies(lax.axis_index("tp") % 2 * half, half, width, gate, up, gate_v, up_v, sem)
    start_all(copies)
    for c in range(n):
        cols = slice(c * width, (c + 1) * width)
        copies[2 * c].wait()
        g_out[:, cols] = jnp.dot(rows[...], gate_v[c], preferred_element_type=jnp.float32)
        copies[2 * c + 1].wait()
        u_out[:, cols] = jnp.dot(rows[...], up_v[c], preferred_element_type=jnp.float32)


def other_body(rows, g_in, u_in, gate, up, down, out, gate_v, up_v, down_v, hid, sem, sem_d):
    n, half, width = gate_v.shape
    n_out, _, width_out = down_v.shape
    copies = half_copies((1 - lax.axis_index("tp") % 2) * half, half, width, gate, up, gate_v, up_v, sem)
    copies_d = [
        pltpu.make_async_copy(down.at[0, :, pl.ds(c * width_out, width_out)], down_v.at[c], sem_d.at[c])
        for c in range(n_out)
    ]
    start_all(copies)
    start_all(copies_d)
    for c in range(n):
        cols = slice(c * width, (c + 1) * width)
        copies[2 * c].wait()
        g = g_in[:, cols] + jnp.dot(rows[...], gate_v[c], preferred_element_type=jnp.float32)
        copies[2 * c + 1].wait()
        u = u_in[:, cols] + jnp.dot(rows[...], up_v[c], preferred_element_type=jnp.float32)
        hid[:, cols] = (g / (1.0 + jnp.exp(-g)) * u).astype(hid.dtype)
    for c in range(n_out):
        copies_d[c].wait()
        out[:, c * width_out : (c + 1) * width_out] = jnp.dot(
            hid[...], down_v[c], preferred_element_type=jnp.float32).astype(out.dtype)


VMEM = pl.BlockSpec(memory_space=pltpu.VMEM)
HBM = pl.BlockSpec(memory_space=pl.ANY)


def own_half(rows, gate, up):
    m, half = rows.shape
    ff = gate.shape[2]
    width = min(CHUNK, ff)
    n = ff // width
    pre = pltpu.VMEM((m, ff), jnp.float32)
    return pl.pallas_call(
        own_body,
        out_shape=[pre, pre],
        in_specs=[VMEM, HBM, HBM],
        out_specs=[VMEM, VMEM],
        scratch_shapes=[
            pltpu.VMEM((n, half, width), gate.dtype),
            pltpu.VMEM((n, half, width), up.dtype),
            pltpu.SemaphoreType.DMA((2 * n,)),
        ],
        cost_estimate=pl.CostEstimate(flops=4 * m * half * ff, bytes_accessed=4 * half * ff, transcendentals=0),
    )(rows, gate, up)


def other_half(rows, g, u, gate, up, down):
    m, half = rows.shape
    ff, d = down.shape[1:]
    width = min(CHUNK, ff)
    n = ff // width
    width_out = min(CHUNK, d)
    n_out = d // width_out
    return pl.pallas_call(
        other_body,
        out_shape=jax.ShapeDtypeStruct((m, d), jnp.bfloat16),
        in_specs=[VMEM, VMEM, VMEM, HBM, HBM, HBM],
        out_specs=VMEM,
        scratch_shapes=[
            pltpu.VMEM((n, half, width), gate.dtype),
            pltpu.VMEM((n, half, width), up.dtype),
            pltpu.VMEM((n_out, ff, width_out), down.dtype),
            pltpu.VMEM((m, ff), jnp.bfloat16),
            pltpu.SemaphoreType.DMA((2 * n,)),
            pltpu.SemaphoreType.DMA((n_out,)),
        ],
    )(rows, g, u, gate, up, down)


def on_device(tokens, chosen, pick_weight, gate_weight, up_weight, down_weight):
    n_tp = lax.axis_size("tp")
    core = lax.axis_index("tp") % 2
    experts, slots = chosen.shape[1:]
    n_tok, d = tokens.shape
    width = d // n_tp
    half = d // 2
    pad = -slots % SUB
    size = slots + pad
    ids = jnp.pad(chosen[0], ((0, 0), (0, pad)), constant_values=-1)
    weight = jnp.pad(pick_weight[0], ((0, 0), (0, pad)))
    positions = lax.iota(jnp.int32, n_tok)
    onehot = (ids.reshape(-1)[:, None] == positions[None, :]).astype(tokens.dtype)
    mine = lax.dynamic_slice_in_dim(tokens, core * half, half, 1)
    picked = jnp.dot(onehot, mine, preferred_element_type=jnp.float32).astype(tokens.dtype)
    own = lax.all_to_all(picked.reshape(experts, size, half), "ep", split_axis=0, concat_axis=0, tiled=True)
    own = own.reshape(-1, half)
    other = lax.ppermute(own, "tp", [(s, s ^ 1) for s in range(n_tp)])
    own = pltpu.with_memory_space_constraint(own, pltpu.VMEM)
    other = pltpu.with_memory_space_constraint(other, pltpu.VMEM)
    g, u = own_half(own, gate_weight, up_weight)
    g = pltpu.with_memory_space_constraint(g, pltpu.VMEM)
    u = pltpu.with_memory_space_constraint(u, pltpu.VMEM)
    part = other_half(other, g, u, gate_weight, up_weight, down_weight)
    part = part.reshape(experts, size, n_tp, width).transpose(0, 2, 1, 3).reshape(experts * n_tp, size, width)
    got = lax.all_to_all(part, ("ep", "tp"), split_axis=0, concat_axis=0, tiled=True).reshape(-1, width)
    spread = jnp.where(positions[:, None, None] == ids[None], weight[None], jnp.zeros((), jnp.float32))
    spread = jnp.broadcast_to(spread[:, :, None, :], (n_tok, experts, n_tp, size)).reshape(n_tok, -1)
    combined = jnp.dot(spread, got.astype(jnp.float32), precision=lax.Precision.HIGHEST, preferred_element_type=jnp.float32)
    return combined.astype(jnp.bfloat16)


def solution(mesh):
    return jax.shard_map(
        on_device,
        mesh=mesh,
        in_specs=(P("ep", None), P("ep", None, None), P("ep", None, None), P("ep", None, "tp"), P("ep", None, "tp"), P("ep", "tp", None)),
        out_specs=P("ep", "tp"),
        check_vma=False,
    )
```
